32 devices in a mesh: sp: 8 (over z, y), fs: 2 (over x), tp: 2 (over core).
Axes of the slice: x: 2, y: 2, z: 4, core: 2. Of those that a mesh axis runs over, the one named last changes fastest.
Arguments:
- ret_query: bfloat16 [1024, 2, 512], P('sp', 'fs', 'tp'), may hold values from -6 to 6
- ret_key: bfloat16 [1024, 2, 512], P('sp', 'fs', 'tp'), may hold values from -6 to 6
- ret_value: bfloat16 [1024, 2, 1024], P('sp', 'fs', 'tp'), may hold values from -6 to 6
- log_decay: float32 [2, 4, 1024], P('fs', 'tp', 'sp'), may hold values from -1.2 to 0
- ret_gain: float32 [1024], P('tp'), may hold values from 0.1 to 1.9
- mla_query: bfloat16 [1024, 2, 1536], P('sp', 'fs', 'tp'), may hold values from -64 to 64
- kv_latent: bfloat16 [1024, 2, 256], P('sp', 'fs'), may hold values from -6 to 6
- rope_key: bfloat16 [1024, 2, 64], P('sp', 'fs'), may hold values from -8 to 8
- key_up: bfloat16 [256, 1024], replicated, may hold values from -0.375 to 0.375
- value_up: bfloat16 [256, 1024], replicated, may hold values from -3 to 3
- ret_out: bfloat16 [1024, 2048], P('tp', 'fs'), may hold values from -0.1875 to 0.1875
- mla_out: bfloat16 [1024, 2048], P('tp', 'fs'), may hold values from -0.1875 to 0.1875
Outputs:
- mixed_rows: bfloat16 [1024, 2, 2048], P(('sp', 'tp'), 'fs')
- log_weight: float32 [2, 8, 1024], P('fs', 'tp', 'sp')
The draws below stay inside these ranges and needn't reach their ends.
All inputs are finite; a program needn't handle non-finite values.
Results may differ from the reference program's by a relative error of at most 0.014.
Values may be sent and summed in bfloat16 or wider, within the bound.
A program may use at most 128 MiB of HBM per device.

```python
import math
import jax
import jax.numpy as jnp
from jax import lax

D = 2048
RH = 4
QK = 128
VD = 256
MH = 8
NOPE = 128
ROPE = 64
VDM = 128
KVR = 256
BLOCK = 128
SEQUENCE_LENGTH = 1024
SEQUENCE_COUNT = 2
N_TP = 2


def draw_log_decay(key, part):
    quick_rate_key, factor_key, spike_key, dropout_key = jax.random.split(jax.random.fold_in(key, 3), 4)
    fast_share = 0.5
    fast_heads = jax.random.uniform(quick_rate_key, (SEQUENCE_COUNT, RH, 1)) < fast_share
    blocks = SEQUENCE_LENGTH // BLOCK
    factor = jax.random.uniform(factor_key, (SEQUENCE_COUNT, RH, blocks), jnp.float32, 0.4, 1.0)
    factor = jnp.repeat(factor, BLOCK, axis=2)
    slow_rate = 0.5 * math.log(10.0) / SEQUENCE_LENGTH
    fast_rate = math.log(10.0) / 40.0
    decay_rates = jnp.where(fast_heads, fast_rate, slow_rate) * factor
    spike_rows = jax.random.randint(spike_key, (SEQUENCE_COUNT, 1, 2), 0, SEQUENCE_LENGTH)
    dropped_entries = jax.random.uniform(dropout_key, (SEQUENCE_COUNT, RH, 2), jnp.float32, 0.2, 0.4)
    total_step_rows = jnp.arange(SEQUENCE_LENGTH)
    removed_mask = total_step_rows[None, None, :, None] == spike_rows[:, :, None, :]
    spike_draws = jnp.sum(jnp.where(removed_mask, jnp.log(1.0 - dropped_entries)[:, :, None, :], 0.0), axis=-1)
    return (spike_draws - decay_rates).astype(jnp.float32)


def draw_rope_key(key, part):
    noise_draw = jax.random.normal(jax.random.fold_in(key, 11), (SEQUENCE_LENGTH, SEQUENCE_COUNT, ROPE), jnp.float32)
    base_draw = jnp.clip(noise_draw, -4.0, 4.0)
    return base_draw.astype(jnp.bfloat16)


def draw_mla_query(key, part):
    noise_draw = jax.random.normal(jax.random.fold_in(key, 13), (SEQUENCE_LENGTH, SEQUENCE_COUNT, MH, NOPE + ROPE), jnp.float32)
    base_draw = jnp.clip(noise_draw, -6.0, 6.0)
    return base_draw.reshape(SEQUENCE_LENGTH, SEQUENCE_COUNT, MH * (NOPE + ROPE)).astype(jnp.bfloat16)


def levels(stream_key, shape, cuts, least, largest):
    loudness, own = 1.0, jax.random.fold_in(stream_key, 6)
    for position, shards_of in cuts:
        steps = jnp.exp(jax.random.uniform(jax.random.fold_in(own, position), (shards_of,), jnp.float32, least / len(cuts), largest / len(cuts)))
        loudness = loudness * jnp.repeat(steps, shape[position] // shards_of).reshape([-1 if axis == position else 1 for axis in range(len(shape))])
    return loudness


def bell_draw(stream_key, shape, deviation, limit, pieces=(), kind=jnp.bfloat16):
    drawn = deviation * jax.random.normal(stream_key, shape, jnp.float32)
    if pieces:
        drawn = drawn * levels(stream_key, shape, pieces, -0.22, 0.18)
    return jnp.clip(drawn, -limit, limit).astype(kind)


def setup_inputs(seed: int = 0) -> dict:
    seeds = jax.random.split(jax.random.key(seed), 13)
    ret_query = bell_draw(seeds[0], (SEQUENCE_LENGTH, SEQUENCE_COUNT, RH * QK), 1.0, 6.0, ((0, 8), (1, 2), (2, 2)))
    ret_key = bell_draw(seeds[1], (SEQUENCE_LENGTH, SEQUENCE_COUNT, RH * QK), 1.0, 6.0, ((0, 8), (1, 2), (2, 2)))
    ret_value = bell_draw(seeds[2], (SEQUENCE_LENGTH, SEQUENCE_COUNT, RH * VD), 1.0, 6.0, ((0, 8), (1, 2), (2, 2)))
    log_decay = draw_log_decay(jax.random.fold_in(seeds[12], 71), 0)
    ret_gain = jnp.clip(1.0 + 0.18 * jax.random.normal(seeds[4], (RH * VD,), jnp.float32), 0.1, 1.9)
    mla_query = draw_mla_query(jax.random.fold_in(seeds[12], 71), 0)
    kv_latent = bell_draw(seeds[6], (SEQUENCE_LENGTH, SEQUENCE_COUNT, KVR), 1.0, 6.0, ((0, 8), (1, 2)))
    rope_key = draw_rope_key(jax.random.fold_in(seeds[12], 71), 0)
    key_up = bell_draw(seeds[8], (KVR, MH * NOPE), KVR ** -0.5, 0.375)
    value_up = bell_draw(seeds[9], (KVR, MH * VDM), 4 ** -0.5, 3.0)
    ret_out = bell_draw(seeds[10], (RH * VD, D), (RH * VD) ** -0.5, 0.1875, ((0, 2), (1, 2)))
    mla_out = bell_draw(seeds[11], (MH * VDM, D), (MH * VDM) ** -0.5, 0.1875, ((0, 2), (1, 2)))
    return dict(ret_query=ret_query, ret_key=ret_key, ret_value=ret_value, log_decay=log_decay, ret_gain=ret_gain, mla_query=mla_query, kv_latent=kv_latent, rope_key=rope_key, key_up=key_up, value_up=value_up, ret_out=ret_out, mla_out=mla_out)


def rotate(vectors, positions):
    half_width = vectors.shape[-1] // 2
    inverse = 1.0 / 10000.0 ** (jnp.arange(half_width, dtype=jnp.float32) / half_width)
    angles = positions.astype(jnp.float32)[:, None] * inverse[None, :]
    cosine = jnp.cos(angles)[:, None, None, :]
    sine_part = jnp.sin(angles)[:, None, None, :]
    widened = vectors.astype(jnp.float32)
    front_part = widened[..., :half_width]
    back_part = widened[..., half_width:]
    turned = jnp.concatenate([front_part * cosine - back_part * sine_part, front_part * sine_part + back_part * cosine], axis=-1)
    return turned.astype(jnp.bfloat16)

def retention_block(state, inputs):
    queries, key_rows, value_rows, decay_rows = inputs
    span_rows = queries.shape[0]
    logit_scale = QK ** (-0.5)
    cumulative = jnp.cumsum(decay_rows, axis=-1)
    log_gap = cumulative[..., :, None] - cumulative[..., None, :]
    causal = jnp.tril(jnp.ones((span_rows, span_rows), dtype=bool))
    score_matrix = jnp.einsum('ishd,jshd->shij', queries.astype(jnp.float32), key_rows.astype(jnp.float32)) * logit_scale
    weights = jnp.where(causal, score_matrix * jnp.exp(jnp.where(causal, log_gap, 0.0)), 0.0).astype(jnp.bfloat16)
    intra_block = jnp.einsum('shij,jshe->ishe', weights.astype(jnp.float32), value_rows.astype(jnp.float32))
    growth = jnp.transpose(jnp.exp(cumulative), (2, 0, 1))[..., None]
    cross_term = jnp.einsum('ishd,shde->ishe', queries.astype(jnp.float32), state, precision=lax.Precision.HIGHEST) * logit_scale * growth
    tail_decay = jnp.transpose(jnp.exp(cumulative[..., -1:] - cumulative), (2, 0, 1))[..., None]
    block_state = jnp.einsum('jshd,jshe->shde', key_rows.astype(jnp.float32) * tail_decay, value_rows.astype(jnp.float32), precision=lax.Precision.HIGHEST)
    next_state = state * jnp.exp(cumulative[..., -1])[..., None, None] + block_state
    return (next_state, intra_block + cross_term)

def reference(ret_query, ret_key, ret_value, log_decay, ret_gain, mla_query, kv_latent, rope_key, key_up, value_up, ret_out, mla_out):
    length = ret_query.shape[0]
    groups = ret_query.shape[1]
    positions = jnp.arange(length, dtype=jnp.int32)
    queries = rotate(ret_query.reshape(length, groups, RH, QK), positions)
    key_rows = rotate(ret_key.reshape(length, groups, RH, QK), positions)
    value_rows = ret_value.reshape(length, groups, RH, VD)
    blocks = length // BLOCK
    decay_blocks = jnp.transpose(log_decay.reshape(groups, RH, blocks, BLOCK), (2, 0, 1, 3))
    initial = jnp.zeros((groups, RH, QK, VD), jnp.float32)
    _, retained = lax.scan(retention_block, initial, (queries.reshape(blocks, BLOCK, groups, RH, QK), key_rows.reshape(blocks, BLOCK, groups, RH, QK), value_rows.reshape(blocks, BLOCK, groups, RH, VD), decay_blocks))
    retained = retained.reshape(length, groups, RH, VD)
    normed = retained * lax.rsqrt(lax.optimization_barrier(jnp.mean(retained * retained, axis=-1, keepdims=True)) + 1e-06) * ret_gain.reshape(RH, VD)
    ret_heads = normed.astype(jnp.bfloat16).reshape(length, groups, RH * VD)
    head_rows = mla_query.reshape(length, groups, MH, NOPE + ROPE)
    query_rope = rotate(head_rows[..., NOPE:], positions)
    key_rope = rotate(rope_key[:, :, None, :], positions)[:, :, 0, :]
    absorbed = jnp.einsum('lshn,chn->lshc', head_rows[..., :NOPE].astype(jnp.float32), key_up.reshape(KVR, MH, NOPE).astype(jnp.float32)).astype(jnp.bfloat16)
    latent_width = kv_latent.astype(jnp.float32)
    rotary_width = key_rope.astype(jnp.float32)
    logit_scale = (NOPE + ROPE) ** (-0.5)
    rows_block = math.gcd(length, 128)

    def query_block(block_index):
        begin_row = block_index * rows_block
        absorbed_block_scores = lax.dynamic_slice_in_dim(absorbed, begin_row, rows_block, 0).astype(jnp.float32)
        rotary_block_scores = lax.dynamic_slice_in_dim(query_rope, begin_row, rows_block, 0).astype(jnp.float32)
        score_matrix = (jnp.einsum('uoda,voa->oduv', absorbed_block_scores, latent_width) + jnp.einsum('covw,zow->ovcz', rotary_block_scores, rotary_width)) * logit_scale
        query_positions = begin_row + jnp.arange(rows_block, dtype=jnp.int32)
        visible = positions[None, :] <= query_positions[:, None]
        score_matrix = jnp.where(visible, score_matrix, -jnp.inf)
        row_max = lax.optimization_barrier(jnp.max(score_matrix, axis=-1))
        exponent = jnp.exp(score_matrix - row_max[..., None])
        total = lax.optimization_barrier(jnp.sum(exponent, axis=-1))
        rounded = lax.optimization_barrier(exponent.astype(jnp.bfloat16))
        weighted = jnp.einsum('shbl,lsc->shbc', rounded.astype(jnp.float32), latent_width)
        latent_mean = (weighted / total[..., None]).astype(jnp.bfloat16)
        return (latent_mean, row_max + jnp.log(total))
    means, log_rows = lax.map(query_block, jnp.arange(length // rows_block, dtype=jnp.int32))
    means = jnp.transpose(means, (1, 2, 0, 3, 4)).reshape(groups, MH, length, KVR)
    log_weight = jnp.transpose(log_rows, (1, 2, 0, 3)).reshape(groups, MH, length)
    mla_heads = jnp.einsum('shlc,chv->lshv', means.astype(jnp.float32), value_up.reshape(KVR, MH, VDM).astype(jnp.float32)).astype(jnp.bfloat16).reshape(length, groups, MH * VDM)
    ret_width = RH * VD // N_TP
    mla_width = MH * VDM // N_TP
    flat_ret = ret_heads.reshape(length * groups, RH * VD)
    flat_mla = mla_heads.reshape(length * groups, MH * VDM)
    summed = jnp.zeros((length * groups, ret_out.shape[1]), jnp.float32)
    for group_index in range(N_TP):
        partial_value = jnp.dot(flat_ret[:, group_index * ret_width:(group_index + 1) * ret_width], ret_out[group_index * ret_width:(group_index + 1) * ret_width], preferred_element_type=jnp.float32)
        partial_value = partial_value + jnp.dot(flat_mla[:, group_index * mla_width:(group_index + 1) * mla_width], mla_out[group_index * mla_width:(group_index + 1) * mla_width], preferred_element_type=jnp.float32)
        rounded_part = lax.optimization_barrier(partial_value.astype(jnp.bfloat16))
        summed = summed + rounded_part.astype(jnp.float32)
    mixed_rows = summed.astype(jnp.bfloat16).reshape(length, groups, ret_out.shape[1])
    return (mixed_rows, log_weight)
```

```python
import functools
import math

import jax
import jax.numpy as jnp
import numpy as np
from jax import lax
from jax.experimental import pallas as pl
from jax.experimental.pallas import tpu as pltpu
from jax.sharding import PartitionSpec as P

QK = 128
VD = 256
NOPE = 128
ROPE = 64
VDM = 128
KVR = 256
KW = 384
MESH = pl.DeviceIdType.MESH
BF = jnp.bfloat16
F32 = jnp.float32


def tables(half, rows, places):
    inverse = 1.0 / 10000.0 ** (np.arange(half) / half)
    inverse = np.concatenate([inverse, inverse])
    near = np.arange(rows)[:, None] * inverse[None, :]
    far = (np.arange(places) * rows)[:, None] * inverse[None, :]
    swap = np.zeros((2 * half, 2 * half), np.float32)
    for j in range(half):
        swap[half + j, j] = -1.0
        swap[j, half + j] = 1.0
    return (
        np.stack([np.cos(near), np.sin(near)]).astype(np.float32),
        np.stack([np.cos(far), np.sin(far)]).astype(np.float32),
        swap,
    )


def dot(a, b):
    return jnp.dot(a, b, preferred_element_type=F32)


def dot_nt(a, b, precision=None):
    return lax.dot_general(
        a, b, (((1,), (1,)), ((), ())), precision=precision, preferred_element_type=F32
    )


def kernel(
    sizes,
    rq_ref, rk_ref, rv_ref, ld_ref, gain_ref, mq_ref, kv_ref, rope_ref,
    near_r, far_r, swap_r, near_m, far_m, swap_m,
    ku_hbm, vu_hbm, ro_hbm, mo_hbm,
    out_ref, lw_ref,
    ku, vu, ro, mo,
    kvb, q_ref, m_ref, l_ref, acc_ref,
    dec_own, dec, st_own, st_in, pre_out, pre_in,
    gath, part, tin, osum, oin, intra_ref, rot_ref, grow_ref,
    w_sem, d_send, d_recv, s_send, s_recv, h_send, h_recv, k_send, k_recv,
    f_send, f_recv, g_send, g_recv, t_send, t_recv, o_send, o_recv,
):
    NP, NF, NT, RL, ML, G = sizes
    stride = NP // G
    rows = rq_ref.shape[0]
    half = rows // NT
    r = st_own.shape[1]
    me = lax.axis_index("sp")
    fs = lax.axis_index("fs")
    tp = lax.axis_index("tp")

    def remote(src, dst, ss, rs, axis, to):
        return pltpu.make_async_remote_copy(
            src_ref=src, dst_ref=dst, send_sem=ss, recv_sem=rs,
            device_id={axis: to}, device_id_type=MESH,
        )

    barrier = pltpu.get_barrier_semaphore()
    for axis, count, own in (("sp", NP, me), ("fs", NF, fs), ("tp", NT, tp)):
        for k in range(1, count):
            pl.semaphore_signal(
                barrier, inc=1, device_id={axis: lax.rem(own + k, count)}, device_id_type=MESH
            )

    wk, wv = ML * NOPE, ML * VDM
    weights = [
        pltpu.make_async_copy(
            ku_hbm.at[:, pl.ds(pl.multiple_of(tp * wk, 128), wk)], ku, w_sem.at[0]
        ),
        pltpu.make_async_copy(
            vu_hbm.at[:, pl.ds(pl.multiple_of(tp * wv, 128), wv)], vu, w_sem.at[1]
        ),
        pltpu.make_async_copy(ro_hbm, ro, w_sem.at[2]),
        pltpu.make_async_copy(mo_hbm, mo, w_sem.at[3]),
    ]
    for copy in weights:
        copy.start()

    def turn(near, far):
        cn, sn = near[0], near[1]
        co, so = far[0, pl.ds(me, 1), :], far[1, pl.ds(me, 1), :]
        return cn * co - sn * so, sn * co + cn * so

    cos_r, sin_r = turn(near_r, far_r)
    cos_m, sin_m = turn(near_m, far_m)

    def rot(x, cosine, sine, swap):
        return (x.astype(F32) * cosine + dot(x, swap[...]) * sine).astype(BF)

    own_rope = rot(rope_ref[...], cos_m, sin_m, swap_m)
    for t in range(NT):
        span = slice(t * half, (t + 1) * half)
        kvb[me, t, :, 0:KVR] = kv_ref[span, :]
        kvb[me, t, :, KVR:KW] = jnp.concatenate(
            [own_rope[span, :], jnp.zeros((half, KW - KVR - ROPE), BF)], axis=-1
        )

    ii = lax.broadcasted_iota(jnp.int32, (rows, rows), 0)
    jj = lax.broadcasted_iota(jnp.int32, (rows, rows), 1)
    low = ii >= jj
    ones_low = jnp.where(low, 1.0, 0.0).astype(F32)
    dec_own[...] = jnp.zeros_like(dec_own)
    dec_own[0:RL, :] = ld_ref[...]
    ld = dec_own[...]
    c_row = dot_nt(ld, ones_low, lax.Precision.HIGHEST)
    c_col = dot_nt(ones_low, ld, lax.Precision.HIGHEST)
    c_end = c_row[:, rows - 1 : rows]
    dec_own[...] = jnp.broadcast_to(jnp.exp(c_end), dec_own.shape)
    states, keys = [], []
    for h in range(RL):
        key = rot(rk_ref[:, h * QK : (h + 1) * QK], cos_r, sin_r, swap_r)
        keys.append(key)
        tail = jnp.exp(c_row[h : h + 1, rows - 1 : rows] - c_col[:, h : h + 1])
        scaled = (key.astype(F32) * tail).T.astype(BF)
        states.append(dot(scaled, rv_ref[:, h * VD : (h + 1) * VD]).astype(BF))
    for g in range(G):
        h, at = divmod(g * r, QK)
        st_own[g] = states[h][at : at + r, :]

    pl.semaphore_wait(barrier, (NP - 1) + (NF - 1) + (NT - 1))

    for g in range(G):
        to = g * stride

        @pl.when(jnp.logical_and(me != to, me < NP - 1))
        def _():
            remote(dec_own, dec.at[me], d_send.at[g], d_recv.at[me], "sp", to).start()
            remote(st_own.at[g], st_in.at[me], s_send.at[g], s_recv.at[me], "sp", to).start()

    def key_copy(to):
        return remote(
            kvb.at[me, tp], kvb.at[me, tp], k_send.at[to], k_recv.at[me], "sp", to
        )

    @pl.loop(1, NP)
    def _(d):
        @pl.when(me + d < NP)
        def _():
            key_copy(me + d).start()

    for h in range(RL):
        query = rot(rq_ref[:, h * QK : (h + 1) * QK], cos_r, sin_r, swap_r)
        rot_ref[h] = query
        gap = jnp.where(low, c_col[:, h : h + 1] - c_row[h : h + 1, :], 0.0)
        w = jnp.where(low, dot_nt(query, keys[h]) * (QK**-0.5) * jnp.exp(gap), 0.0).astype(BF)
        intra_ref[h] = dot(w, rv_ref[:, h * VD : (h + 1) * VD])
        grow_ref[h] = jnp.broadcast_to(
            jnp.exp(c_col[:, h : h + 1]) * (QK**-0.5), (rows, 128)
        )

    weights[0].wait()
    weights[1].wait()
    mq = mq_ref[...]
    width = NOPE + ROPE
    for h in range(ML):
        nope = mq[:, h * width : h * width + NOPE]
        span = slice(h * rows, (h + 1) * rows)
        q_ref[span, 0:KVR] = dot_nt(nope, ku[:, h * NOPE : (h + 1) * NOPE]).astype(BF)
        turned = rot(mq[:, h * width + NOPE : (h + 1) * width], cos_m, sin_m, swap_m)
        q_ref[span, KVR:KW] = jnp.concatenate(
            [turned, jnp.zeros((rows, KW - KVR - ROPE), BF)], axis=-1
        )

    def scores(at):
        block = kvb[at].reshape(rows, KW)
        return dot_nt(q_ref[...], block) * (width**-0.5), block[:, 0:KVR]

    s, latent = scores(me)
    hide = jnp.where(low, 0.0, -1e30).astype(F32)
    s = s + jnp.concatenate([hide] * ML, axis=0)
    top = jnp.max(s, axis=-1, keepdims=True)
    e = jnp.exp(s - top)
    m_ref[...] = jnp.broadcast_to(top, m_ref.shape)
    l_ref[...] = jnp.broadcast_to(jnp.sum(e, axis=-1, keepdims=True), l_ref.shape)
    acc_ref[...] = dot(e.astype(BF), latent)

    @pl.when(lax.rem(me, stride) == 0)
    def _():
        g = lax.div(me, stride)
        head = lax.div(g * r, QK)
        st_in[me] = st_own[g]
        dec[me] = dec_own[...]

        def scan(n, pre):
            pre_out[n] = pre.astype(BF)

            @pl.when(jnp.logical_and(n > 0, n != me))
            def _():
                remote(pre_out.at[n], pre_in.at[g], h_send.at[n], h_recv.at[g], "sp", n).start()

            @pl.when(jnp.logical_and(n < NP - 1, n != me))
            def _():
                remote(dec_own, dec.at[n], d_send.at[0], d_recv.at[n], "sp", n).wait_recv()
                remote(st_own.at[0], st_in.at[n], s_send.at[0], s_recv.at[n], "sp", n).wait_recv()

            factor = dec[n, pl.ds(head, 1), 0:1]
            return pre * factor + st_in[n].astype(F32)

        last = lax.fori_loop(0, NP - 1, scan, jnp.zeros((r, VD), F32))
        pre_out[NP - 1] = last.astype(BF)

        @pl.when(me != NP - 1)
        def _():
            remote(
                pre_out.at[NP - 1], pre_in.at[g], h_send.at[NP - 1], h_recv.at[g], "sp", NP - 1
            ).start()

        pre_in[g] = pre_out[me]

    def forward(at, k):
        to = lax.rem(tp + k, NT)
        return remote(
            kvb.at[at, tp], kvb.at[at, tp], f_send.at[k, at], f_recv.at[tp, at], "tp", to
        )

    @pl.loop(1, NP + 1)
    def _(d):
        @pl.when(d <= me)
        def _():
            at = me - d
            remote(kvb.at[at, tp], kvb.at[at, tp], k_send.at[at], k_recv.at[at], "sp", at).wait_recv()
            for k in range(1, NT):
                forward(at, k).start()

        @pl.when(jnp.logical_and(d >= 2, d - 1 <= me))
        def _():
            at = me - d + 1
            for k in range(1, NT):
                src = lax.rem(tp + k, NT)
                remote(
                    kvb.at[at, src], kvb.at[at, src], f_send.at[k, at], f_recv.at[src, at], "tp", src
                ).wait_recv()
            s, latent = scores(at)
            before = m_ref[:, 0:1]
            top = jnp.maximum(before, jnp.max(s, axis=-1, keepdims=True))
            e = jnp.exp(s - top)
            shrink = jnp.exp(before - top)
            total = l_ref[:, 0:1] * shrink + jnp.sum(e, axis=-1, keepdims=True)
            m_ref[...] = jnp.broadcast_to(top, m_ref.shape)
            l_ref[...] = jnp.broadcast_to(total, l_ref.shape)
            acc_ref[...] = acc_ref[...] * shrink + dot(e.astype(BF), latent)

    def heads_copy(kind, k):
        to = lax.rem(fs + k, NF)
        return remote(
            gath.at[fs, kind], gath.at[fs, kind], g_send.at[k, kind], g_recv.at[fs, kind], "fs", to
        )

    for h in range(ML):
        span = slice(h * rows, (h + 1) * rows)
        total = l_ref[span, :]
        mean = (acc_ref[span, :] / total[:, 0:1]).astype(BF)
        gath[fs, 1, :, h * VDM : (h + 1) * VDM] = dot(mean, vu[:, h * VDM : (h + 1) * VDM]).astype(BF)
        lw_ref[h : h + 1, :] = (m_ref[span, :] + jnp.log(total)).T[0:1, :]
    for k in range(1, NF):
        heads_copy(1, k).start()

    @pl.when(me > 0)
    def _():
        for g in range(G):
            @pl.when(me != g * stride)
            def _():
                remote(
                    pre_out.at[0], pre_in.at[g], h_send.at[0], h_recv.at[g], "sp", g * stride
                ).wait_recv()

    @pl.when(me == 0)
    def _():
        pre_in[...] = jnp.zeros_like(pre_in)

    per = G // RL
    for h in range(RL):
        state = pre_in[h * per : (h + 1) * per].reshape(QK, VD)
        kept = intra_ref[h] + dot(rot_ref[h], state) * grow_ref[h][:, 0:1]
        normed = kept * lax.rsqrt(jnp.mean(kept * kept, axis=-1, keepdims=True) + 1e-06)
        normed = normed * gain_ref[0:1, h * VD : (h + 1) * VD]
        gath[fs, 0, :, h * VD : (h + 1) * VD] = normed.astype(BF)
    for k in range(1, NF):
        heads_copy(0, k).start()

    weights[2].wait()
    weights[3].wait()

    def partial_copy(s, k):
        to = lax.rem(tp + k, NT)
        return remote(part.at[s, to], tin.at[tp, s], t_send.at[k, s], t_recv.at[tp, s], "tp", to)

    def project(s):
        whole = (dot(gath[s, 1], mo[...]) + dot(gath[s, 0], ro[...])).astype(BF)
        for t in range(NT):
            part[s, t] = whole[t * half : (t + 1) * half, :]
        for k in range(1, NT):
            partial_copy(s, k).start()

    def summed(s):
        total = part[s, tp].astype(F32)
        for k in range(1, NT):
            src = lax.rem(tp + k, NT)
            remote(part.at[s, 0], tin.at[src, s], t_send.at[k, s], t_recv.at[src, s], "tp", src).wait_recv()
            total = total + tin[src, s].astype(F32)
        return total.astype(BF)

    project(fs)
    own = summed(fs)
    cols = out_ref.shape[1] // NF
    for k in range(1, NF):
        s = lax.rem(fs + k, NF)
        for kind in (1, 0):
            remote(
                gath.at[s, kind], gath.at[s, kind], g_send.at[k, kind], g_recv.at[s, kind], "fs", s
            ).wait_recv()
        project(s)

    def back_copy(k):
        s = lax.rem(fs + k, NF)
        return remote(osum.at[s], oin.at[fs], o_send.at[k], o_recv.at[fs], "fs", s)

    for k in range(1, NF):
        s = lax.rem(fs + k, NF)
        osum[s] = summed(s)
        back_copy(k).start()
    out_ref[:, pl.ds(pl.multiple_of(fs * cols, 128), cols)] = own

    for g in range(G):
        @pl.when(jnp.logical_and(me != g * stride, me < NP - 1))
        def _():
            remote(dec_own, dec.at[me], d_send.at[g], d_recv.at[me], "sp", g * stride).wait_send()
            remote(st_own.at[g], st_in.at[me], s_send.at[g], s_recv.at[me], "sp", g * stride).wait_send()

    @pl.loop(1, NP)
    def _(d):
        @pl.when(me + d < NP)
        def _():
            key_copy(me + d).wait_send()

        @pl.when(d <= me)
        def _():
            for k in range(1, NT):
                forward(me - d, k).wait_send()

        @pl.when(jnp.logical_and(lax.rem(me, stride) == 0, d != me))
        def _():
            g = lax.div(me, stride)
            remote(pre_out.at[d], pre_in.at[g], h_send.at[d], h_recv.at[g], "sp", d).wait_send()

    for k in range(1, NF):
        for kind in range(2):
            heads_copy(kind, k).wait_send()
    for s in range(NF):
        for k in range(1, NT):
            partial_copy(s, k).wait_send()
    for k in range(1, NF):
        back_copy(k).wait_send()
    for k in range(1, NF):
        s = lax.rem(fs + k, NF)
        remote(osum.at[s], oin.at[s], o_send.at[k], o_recv.at[s], "fs", s).wait_recv()
        out_ref[:, pl.ds(pl.multiple_of(s * cols, 128), cols)] = oin[s]


def on_device(
    counts,
    ret_query, ret_key, ret_value, log_decay, ret_gain, mla_query,
    kv_latent, rope_key, key_up, value_up, ret_out, mla_out,
):
    NP, NF, NT = counts
    rows = ret_query.shape[0]
    RL = ret_value.shape[2] // VD
    ML = mla_query.shape[2] // (NOPE + ROPE)
    G = min(NP, RL * QK // 16)
    r = RL * QK // G
    half = rows // NT
    cols = ret_out.shape[1]
    near_r, far_r, swap_r = tables(QK // 2, rows, NP)
    near_m, far_m, swap_m = tables(ROPE // 2, rows, NP)
    flat = lambda a: a.reshape(rows, a.shape[2])
    vm = pl.BlockSpec(memory_space=pltpu.VMEM)
    hbm = pl.BlockSpec(memory_space=pl.ANY)
    V = pltpu.VMEM
    D = pltpu.SemaphoreType.DMA
    out, lw = pl.pallas_call(
        functools.partial(kernel, (NP, NF, NT, RL, ML, G)),
        out_shape=(
            jax.ShapeDtypeStruct((half, cols * NF), BF),
            jax.ShapeDtypeStruct((ML, rows), F32),
        ),
        in_specs=[vm] * 14 + [hbm] * 4,
        out_specs=(vm, vm),
        scratch_shapes=[
            V((KVR, ML * NOPE), BF), V((KVR, ML * VDM), BF),
            V(ret_out.shape, BF), V(mla_out.shape, BF),
            V((NP, NT, half, KW), BF), V((ML * rows, KW), BF),
            V((ML * rows, 128), F32), V((ML * rows, 128), F32), V((ML * rows, KVR), F32),
            V((8, 128), F32), V((NP, 8, 128), F32),
            V((G, r, VD), BF), V((NP, r, VD), BF), V((NP, r, VD), BF), V((G, r, VD), BF),
            V((NF, 2, rows, ML * VDM), BF), V((NF, NT, half, cols), BF),
            V((NT, NF, half, cols), BF), V((NF, half, cols), BF), V((NF, half, cols), BF),
            V((RL, rows, VD), F32), V((RL, rows, QK), BF), V((RL, rows, 128), F32),
            D((4,)), D((G,)), D((NP,)), D((G,)), D((NP,)), D((NP,)), D((G,)), D((NP,)), D((NP,)),
            D((NT, NP)), D((NT, NP)), D((NF, 2)), D((NF, 2)), D((NT, NF)), D((NT, NF)),
            D((NF,)), D((NF,)),
        ],
        compiler_params=pltpu.CompilerParams(collective_id=0, has_side_effects=True),
    )(
        flat(ret_query), flat(ret_key), flat(ret_value), log_decay.reshape(RL, rows),
        ret_gain.reshape(1, RL * VD), flat(mla_query), flat(kv_latent), flat(rope_key),
        jnp.asarray(near_r), jnp.asarray(far_r), jnp.asarray(swap_r, BF),
        jnp.asarray(near_m), jnp.asarray(far_m), jnp.asarray(swap_m, BF),
        key_up, value_up, ret_out, mla_out,
    )
    return out.reshape(half, 1, cols * NF), lw.reshape(1, ML, rows)


def solution(mesh):
    counts = tuple(mesh.shape[a] for a in ("sp", "fs", "tp"))
    wide = P("sp", "fs", "tp")
    in_specs = (
        wide, wide, wide, P("fs", "tp", "sp"), P("tp"), wide,
        P("sp", "fs", None), P("sp", "fs", None), P(), P(), P("tp", "fs"), P("tp", "fs"),
    )
    out_specs = (P(("sp", "tp"), "fs", None), P("fs", "tp", "sp"))
    return jax.shard_map(
        functools.partial(on_device, counts),
        mesh=mesh, in_specs=in_specs, out_specs=out_specs, check_vma=False,
    )
```

```python
import functools
import math

import jax
import jax.numpy as jnp
import numpy as np
from jax import lax
from jax.experimental import pallas as pl
from jax.experimental.pallas import tpu as pltpu
from jax.sharding import PartitionSpec as P

QK = 128
VD = 256
NOPE = 128
ROPE = 64
VDM = 128
KVR = 256
KW = 384
MESH = pl.DeviceIdType.MESH
BF = jnp.bfloat16
F32 = jnp.float32


def tables(half, rows, places):
    inverse = 1.0 / 10000.0 ** (np.arange(half) / half)
    inverse = np.concatenate([inverse, inverse])
    near = np.arange(rows)[:, None] * inverse[None, :]
    far = (np.arange(places) * rows)[:, None] * inverse[None, :]
    swap = np.zeros((2 * half, 2 * half), np.float32)
    for j in range(half):
        swap[half + j, j] = -1.0
        swap[j, half + j] = 1.0
    return (
        np.stack([np.cos(near), np.sin(near)]).astype(np.float32),
        np.stack([np.cos(far), np.sin(far)]).astype(np.float32),
        swap,
    )


def dot(a, b):
    return jnp.dot(a, b, preferred_element_type=F32)


def dot_nt(a, b, precision=None):
    return lax.dot_general(
        a, b, (((1,), (1,)), ((), ())), precision=precision, preferred_element_type=F32
    )


def kernel(
    sizes,
    rq_ref, rk_ref, rv_ref, ld_ref, gain_ref, mq_ref, kv_ref, rope_ref,
    near_r, far_r, swap_r, near_m, far_m, swap_m,
    ku_hbm, vu_hbm, ro_hbm, mo_hbm,
    out_ref, lw_ref,
    ku, vu, ro, mo,
    kvb, q_ref, m_ref, l_ref, acc_ref,
    dec_own, dec, st_own, st_in, pre_out, pre_in,
    gath, part, tin, osum, oin, intra_ref, rot_ref, grow_ref,
    w_sem, d_send, d_recv, s_send, s_recv, h_send, h_recv, k_send, k_recv,
    f_send, f_recv, y_send, g_send, g_recv, t_send, t_recv, o_send, o_recv,
):
    NP, NF, NT, RL, ML, G = sizes
    stride = NP // G
    NY = max(i for i in range(1, math.isqrt(NP) + 1) if NP % i == 0)
    NZ = NP // NY
    rows = rq_ref.shape[0]
    half = rows // NT
    r = st_own.shape[1]
    me = lax.axis_index("sp")
    fs = lax.axis_index("fs")
    tp = lax.axis_index("tp")
    z, y = lax.div(me, NY), lax.rem(me, NY)

    def remote(src, dst, ss, rs, axis, to):
        return pltpu.make_async_remote_copy(
            src_ref=src, dst_ref=dst, send_sem=ss, recv_sem=rs,
            device_id={axis: to}, device_id_type=MESH,
        )

    barrier = pltpu.get_barrier_semaphore()
    for axis, count, own in (("sp", NP, me), ("fs", NF, fs), ("tp", NT, tp)):
        for k in range(1, count):
            pl.semaphore_signal(
                barrier, inc=1, device_id={axis: lax.rem(own + k, count)}, device_id_type=MESH
            )

    wk, wv = ML * NOPE, ML * VDM
    weights = [
        pltpu.make_async_copy(
            ku_hbm.at[:, pl.ds(pl.multiple_of(tp * wk, 128), wk)], ku, w_sem.at[0]
        ),
        pltpu.make_async_copy(
            vu_hbm.at[:, pl.ds(pl.multiple_of(tp * wv, 128), wv)], vu, w_sem.at[1]
        ),
        pltpu.make_async_copy(ro_hbm, ro, w_sem.at[2]),
        pltpu.make_async_copy(mo_hbm, mo, w_sem.at[3]),
    ]
    for copy in weights:
        copy.start()

    def turn(near, far):
        cn, sn = near[0], near[1]
        co, so = far[0, pl.ds(me, 1), :], far[1, pl.ds(me, 1), :]
        return cn * co - sn * so, sn * co + cn * so

    cos_r, sin_r = turn(near_r, far_r)
    cos_m, sin_m = turn(near_m, far_m)

    def rot(x, cosine, sine, swap):
        return (x.astype(F32) * cosine + dot(x, swap[...]) * sine).astype(BF)

    own_rope = rot(rope_ref[...].astype(F32).T.astype(BF), cos_m, sin_m, swap_m)
    for t in range(NT):
        span = slice(t * half, (t + 1) * half)
        kvb[me, t, :, 0:KVR] = kv_ref[span, :]
        kvb[me, t, :, KVR:KW] = jnp.concatenate(
            [own_rope[span, :], jnp.zeros((half, KW - KVR - ROPE), BF)], axis=-1
        )

    ii = lax.broadcasted_iota(jnp.int32, (rows, rows), 0)
    jj = lax.broadcasted_iota(jnp.int32, (rows, rows), 1)
    low = ii >= jj
    ones_low = jnp.where(low, 1.0, 0.0).astype(F32)
    dec_own[...] = jnp.zeros_like(dec_own)
    dec_own[0:RL, :] = ld_ref[...]
    ld = dec_own[...]
    c_row = dot_nt(ld, ones_low, lax.Precision.HIGHEST)
    c_col = dot_nt(ones_low, ld, lax.Precision.HIGHEST)
    c_end = c_row[:, rows - 1 : rows]
    dec_own[...] = jnp.broadcast_to(jnp.exp(c_end), dec_own.shape)
    states, keys = [], []
    for h in range(RL):
        key = rot(rk_ref[:, h * QK : (h + 1) * QK], cos_r, sin_r, swap_r)
        keys.append(key)
        tail = jnp.exp(c_row[h : h + 1, rows - 1 : rows] - c_col[:, h : h + 1])
        scaled = (key.astype(F32) * tail).T.astype(BF)
        states.append(dot(scaled, rv_ref[:, h * VD : (h + 1) * VD]).astype(BF))
    for g in range(G):
        h, at = divmod(g * r, QK)
        st_own[g] = states[h][at : at + r, :]

    pl.semaphore_wait(barrier, (NP - 1) + (NF - 1) + (NT - 1))

    for g in range(G):
        to = g * stride

        @pl.when(jnp.logical_and(me != to, me < NP - 1))
        def _():
            remote(dec_own, dec.at[me], d_send.at[g], d_recv.at[me], "sp", to).start()
            remote(st_own.at[g], st_in.at[me], s_send.at[g], s_recv.at[me], "sp", to).start()

    def key_copy(to):
        return remote(
            kvb.at[me, tp], kvb.at[me, tp], k_send.at[to], k_recv.at[me], "sp", to
        )

    def key_targets(act):
        for k in range(1, NY):
            @pl.when(y + k < NY)
            def _():
                act(key_copy(me + k))

        @pl.loop(1, NZ)
        def _(d):
            @pl.when(z + d < NZ)
            def _():
                act(key_copy(me + d * NY))

    key_targets(lambda copy: copy.start())

    for h in range(RL):
        query = rot(rq_ref[:, h * QK : (h + 1) * QK], cos_r, sin_r, swap_r)
        rot_ref[h] = query
        gap = jnp.where(low, c_col[:, h : h + 1] - c_row[h : h + 1, :], 0.0)
        w = jnp.where(low, dot_nt(query, keys[h]) * (QK**-0.5) * jnp.exp(gap), 0.0).astype(BF)
        intra_ref[h] = dot(w, rv_ref[:, h * VD : (h + 1) * VD])
        grow_ref[h] = jnp.broadcast_to(
            jnp.exp(c_col[:, h : h + 1]) * (QK**-0.5), (rows, 128)
        )

    weights[0].wait()
    weights[1].wait()
    mq = mq_ref[...]
    width = NOPE + ROPE
    for h in range(ML):
        nope = mq[:, h * width : h * width + NOPE]
        span = slice(h * rows, (h + 1) * rows)
        q_ref[span, 0:KVR] = dot_nt(nope, ku[:, h * NOPE : (h + 1) * NOPE]).astype(BF)
        turned = rot(mq[:, h * width + NOPE : (h + 1) * width], cos_m, sin_m, swap_m)
        q_ref[span, KVR:KW] = jnp.concatenate(
            [turned, jnp.zeros((rows, KW - KVR - ROPE), BF)], axis=-1
        )

    def scores(at):
        block = kvb[at].reshape(rows, KW)
        return dot_nt(q_ref[...], block) * (width**-0.5), block[:, 0:KVR]

    s, latent = scores(me)
    hide = jnp.where(low, 0.0, -1e30).astype(F32)
    s = s + jnp.concatenate([hide] * ML, axis=0)
    top = jnp.max(s, axis=-1, keepdims=True)
    e = jnp.exp(s - top)
    m_ref[...] = jnp.broadcast_to(top, m_ref.shape)
    l_ref[...] = jnp.broadcast_to(jnp.sum(e, axis=-1, keepdims=True), l_ref.shape)
    acc_ref[...] = dot(e.astype(BF), latent)

    @pl.when(lax.rem(me, stride) == 0)
    def _():
        g = lax.div(me, stride)
        head = lax.div(g * r, QK)
        st_in[me] = st_own[g]
        dec[me] = dec_own[...]

        def scan(n, pre):
            pre_out[n] = pre.astype(BF)

            @pl.when(jnp.logical_and(n > 0, n != me))
            def _():
                remote(pre_out.at[n], pre_in.at[g], h_send.at[n], h_recv.at[g], "sp", n).start()

            @pl.when(jnp.logical_and(n < NP - 1, n != me))
            def _():
                remote(dec_own, dec.at[n], d_send.at[0], d_recv.at[n], "sp", n).wait_recv()
                remote(st_own.at[0], st_in.at[n], s_send.at[0], s_recv.at[n], "sp", n).wait_recv()

            factor = dec[n, pl.ds(head, 1), 0:1]
            return pre * factor + st_in[n].astype(F32)

        last = lax.fori_loop(0, NP - 1, scan, jnp.zeros((r, VD), F32))
        pre_out[NP - 1] = last.astype(BF)

        @pl.when(me != NP - 1)
        def _():
            remote(
                pre_out.at[NP - 1], pre_in.at[g], h_send.at[NP - 1], h_recv.at[g], "sp", NP - 1
            ).start()

        pre_in[g] = pre_out[me]

    def forward(at, k):
        to = lax.rem(tp + k, NT)
        return remote(
            kvb.at[at, tp], kvb.at[at, tp], f_send.at[k, at], f_recv.at[tp, at], "tp", to
        )

    def relay(at, k):
        to = z * NY + lax.rem(y + k, NY)
        return remote(
            kvb.at[at, tp], kvb.at[at, tp], y_send.at[k, at], k_recv.at[at], "sp", to
        )

    def landed(at):
        remote(kvb.at[at, tp], kvb.at[at, tp], k_send.at[at], k_recv.at[at], "sp", at).wait_recv()
        for k in range(1, NT):
            forward(at, k).start()

    def paired(at):
        for k in range(1, NT):
            src = lax.rem(tp + k, NT)
            remote(
                kvb.at[at, src], kvb.at[at, src], f_send.at[k, at], f_recv.at[src, at], "tp", src
            ).wait_recv()

    def attend(block):
        s = dot_nt(q_ref[...], block) * (width**-0.5)
        before = m_ref[:, 0:1]
        top = jnp.maximum(before, jnp.max(s, axis=-1, keepdims=True))
        e = jnp.exp(s - top)
        shrink = jnp.exp(before - top)
        total = l_ref[:, 0:1] * shrink + jnp.sum(e, axis=-1, keepdims=True)
        m_ref[...] = jnp.broadcast_to(top, m_ref.shape)
        l_ref[...] = jnp.broadcast_to(total, l_ref.shape)
        acc_ref[...] = acc_ref[...] * shrink + dot(e.astype(BF), block[:, 0:KVR])

    def direct(j):
        @pl.when(j <= z)
        def _():
            at = me - j * NY
            landed(at)
            for k in range(1, NY):
                relay(at, k).start()

    direct(1)
    for k in range(1, NY):
        @pl.when(y >= k)
        def _():
            landed(me - k)

    for k in range(1, NY):
        @pl.when(y >= k)
        def _():
            paired(me - k)
            attend(kvb[me - k].reshape(rows, KW))

    def line(j):
        direct(j + 1)

        @pl.when(j <= z)
        def _():
            first = (z - j) * NY
            for k in range(1, NY):
                landed(first + lax.rem(y + k, NY))
            for k in range(NY):
                paired(first + lax.rem(y + k, NY))
            attend(kvb[pl.ds(first, NY)].reshape(NY * rows, KW))

    split = max(NZ // 2, 1)

    @pl.loop(1, split)
    def _(j):
        line(j)

    def heads_copy(kind, k):
        to = lax.rem(fs + k, NF)
        return remote(
            gath.at[fs, kind], gath.at[fs, kind], g_send.at[k, kind], g_recv.at[fs, kind], "fs", to
        )

    @pl.when(me > 0)
    def _():
        for g in range(G):
            @pl.when(me != g * stride)
            def _():
                remote(
                    pre_out.at[0], pre_in.at[g], h_send.at[0], h_recv.at[g], "sp", g * stride
                ).wait_recv()

    @pl.when(me == 0)
    def _():
        pre_in[...] = jnp.zeros_like(pre_in)

    per = G // RL
    for h in range(RL):
        state = pre_in[h * per : (h + 1) * per].reshape(QK, VD)
        kept = intra_ref[h] + dot(rot_ref[h], state) * grow_ref[h][:, 0:1]
        normed = kept * lax.rsqrt(jnp.mean(kept * kept, axis=-1, keepdims=True) + 1e-06)
        normed = normed * gain_ref[0:1, h * VD : (h + 1) * VD]
        gath[fs, 0, :, h * VD : (h + 1) * VD] = normed.astype(BF)
    for k in range(1, NF):
        heads_copy(0, k).start()

    @pl.loop(split, NZ)
    def _(j):
        line(j)

    for h in range(ML):
        span = slice(h * rows, (h + 1) * rows)
        total = l_ref[span, :]
        mean = (acc_ref[span, :] / total[:, 0:1]).astype(BF)
        gath[fs, 1, :, h * VDM : (h + 1) * VDM] = dot(mean, vu[:, h * VDM : (h + 1) * VDM]).astype(BF)
        lw_ref[h : h + 1, :] = (m_ref[span, :] + jnp.log(total)).T[0:1, :]
    for k in range(1, NF):
        heads_copy(1, k).start()

    weights[2].wait()
    weights[3].wait()

    def partial_copy(s, k):
        to = lax.rem(tp + k, NT)
        return remote(part.at[s, to], tin.at[tp, s], t_send.at[k, s], t_recv.at[tp, s], "tp", to)

    def project(s):
        whole = (dot(gath[s, 1], mo[...]) + dot(gath[s, 0], ro[...])).astype(BF)
        for t in range(NT):
            part[s, t] = whole[t * half : (t + 1) * half, :]
        for k in range(1, NT):
            partial_copy(s, k).start()

    def summed(s):
        total = part[s, tp].astype(F32)
        for k in range(1, NT):
            src = lax.rem(tp + k, NT)
            remote(part.at[s, 0], tin.at[src, s], t_send.at[k, s], t_recv.at[src, s], "tp", src).wait_recv()
            total = total + tin[src, s].astype(F32)
        return total.astype(BF)

    project(fs)
    own = summed(fs)
    cols = out_ref.shape[1] // NF
    for k in range(1, NF):
        s = lax.rem(fs + k, NF)
        for kind in (0, 1):
            remote(
                gath.at[s, kind], gath.at[s, kind], g_send.at[k, kind], g_recv.at[s, kind], "fs", s
            ).wait_recv()
        project(s)

    def back_copy(k):
        s = lax.rem(fs + k, NF)
        return remote(osum.at[s], oin.at[fs], o_send.at[k], o_recv.at[fs], "fs", s)

    for k in range(1, NF):
        s = lax.rem(fs + k, NF)
        osum[s] = summed(s)
        back_copy(k).start()
    out_ref[:, pl.ds(pl.multiple_of(fs * cols, 128), cols)] = own

    key_targets(lambda copy: copy.wait_send())

    @pl.loop(1, NZ)
    def _(j):
        @pl.when(j <= z)
        def _():
            for k in range(1, NY):
                relay(me - j * NY, k).wait_send()

    for g in range(G):
        @pl.when(jnp.logical_and(me != g * stride, me < NP - 1))
        def _():
            remote(dec_own, dec.at[me], d_send.at[g], d_recv.at[me], "sp", g * stride).wait_send()
            remote(st_own.at[g], st_in.at[me], s_send.at[g], s_recv.at[me], "sp", g * stride).wait_send()

    @pl.loop(1, NP)
    def _(d):
        @pl.when(d <= me)
        def _():
            for k in range(1, NT):
                forward(me - d, k).wait_send()

        @pl.when(jnp.logical_and(lax.rem(me, stride) == 0, d != me))
        def _():
            g = lax.div(me, stride)
            remote(pre_out.at[d], pre_in.at[g], h_send.at[d], h_recv.at[g], "sp", d).wait_send()

    for k in range(1, NF):
        for kind in range(2):
            heads_copy(kind, k).wait_send()
    for s in range(NF):
        for k in range(1, NT):
            partial_copy(s, k).wait_send()
    for k in range(1, NF):
        back_copy(k).wait_send()
    for k in range(1, NF):
        s = lax.rem(fs + k, NF)
        remote(osum.at[s], oin.at[s], o_send.at[k], o_recv.at[s], "fs", s).wait_recv()
        out_ref[:, pl.ds(pl.multiple_of(s * cols, 128), cols)] = oin[s]


def on_device(
    counts,
    ret_query, ret_key, ret_value, log_decay, ret_gain, mla_query,
    kv_latent, rope_key, key_up, value_up, ret_out, mla_out,
):
    NP, NF, NT = counts
    rows = ret_query.shape[0]
    RL = ret_value.shape[2] // VD
    ML = mla_query.shape[2] // (NOPE + ROPE)
    G = min(NP, RL * QK // 16)
    r = RL * QK // G
    lines = max(i for i in range(1, math.isqrt(NP) + 1) if NP % i == 0)
    half = rows // NT
    cols = ret_out.shape[1]
    near_r, far_r, swap_r = tables(QK // 2, rows, NP)
    near_m, far_m, swap_m = tables(ROPE // 2, rows, NP)
    flat = lambda a: a.reshape(rows, a.shape[2])
    vm = pl.BlockSpec(memory_space=pltpu.VMEM)
    hbm = pl.BlockSpec(memory_space=pl.ANY)
    V = pltpu.VMEM
    D = pltpu.SemaphoreType.DMA
    out, lw = pl.pallas_call(
        functools.partial(kernel, (NP, NF, NT, RL, ML, G)),
        out_shape=(
            jax.ShapeDtypeStruct((half, cols * NF), BF),
            jax.ShapeDtypeStruct((ML, rows), F32),
        ),
        in_specs=[vm] * 14 + [hbm] * 4,
        out_specs=(vm, vm),
        scratch_shapes=[
            V((KVR, ML * NOPE), BF), V((KVR, ML * VDM), BF),
            V(ret_out.shape, BF), V(mla_out.shape, BF),
            V((NP, NT, half, KW), BF), V((ML * rows, KW), BF),
            V((ML * rows, 128), F32), V((ML * rows, 128), F32), V((ML * rows, KVR), F32),
            V((8, 128), F32), V((NP, 8, 128), F32),
            V((G, r, VD), BF), V((NP, r, VD), BF), V((NP, r, VD), BF), V((G, r, VD), BF),
            V((NF, 2, rows, ML * VDM), BF), V((NF, NT, half, cols), BF),
            V((NT, NF, half, cols), BF), V((NF, half, cols), BF), V((NF, half, cols), BF),
            V((RL, rows, VD), F32), V((RL, rows, QK), BF), V((RL, rows, 128), F32),
            D((4,)), D((G,)), D((NP,)), D((G,)), D((NP,)), D((NP,)), D((G,)), D((NP,)), D((NP,)),
            D((NT, NP)), D((NT, NP)), D((lines, NP)), D((NF, 2)), D((NF, 2)), D((NT, NF)), D((NT, NF)),
            D((NF,)), D((NF,)),
        ],
        compiler_params=pltpu.CompilerParams(collective_id=0, has_side_effects=True),
    )(
        flat(ret_query), flat(ret_key), flat(ret_value), log_decay.reshape(RL, rows),
        ret_gain.reshape(1, RL * VD), flat(mla_query), flat(kv_latent), flat(rope_key).T,
        jnp.asarray(near_r), jnp.asarray(far_r), jnp.asarray(swap_r, BF),
        jnp.asarray(near_m), jnp.asarray(far_m), jnp.asarray(swap_m, BF),
        key_up, value_up, ret_out, mla_out,
    )
    return out.reshape(half, 1, cols * NF), lw.reshape(1, ML, rows)


def solution(mesh):
    counts = tuple(mesh.shape[a] for a in ("sp", "fs", "tp"))
    wide = P("sp", "fs", "tp")
    in_specs = (
        wide, wide, wide, P("fs", "tp", "sp"), P("tp"), wide,
        P("sp", "fs", None), P("sp", "fs", None), P(), P(), P("tp", "fs"), P("tp", "fs"),
    )
    out_specs = (P(("sp", "tp"), "fs", None), P("fs", "tp", "sp"))
    return jax.shard_map(
        functools.partial(on_device, counts),
        mesh=mesh, in_specs=in_specs, out_specs=out_specs, check_vma=False,
    )
```

```python
import functools
import math

import jax
import jax.numpy as jnp
import numpy as np
from jax import lax
from jax.experimental import pallas as pl
from jax.experimental.pallas import tpu as pltpu
from jax.sharding import PartitionSpec as P

QK = 128
VD = 256
NOPE = 128
ROPE = 64
VDM = 128
KVR = 256
KW = 384
CUTS = 2
MESH = pl.DeviceIdType.MESH
BF = jnp.bfloat16
F32 = jnp.float32


def tables(half, rows, places):
    inverse = 1.0 / 10000.0 ** (np.arange(half) / half)
    inverse = np.concatenate([inverse, inverse])
    near = np.arange(rows)[:, None] * inverse[None, :]
    far = (np.arange(places) * rows)[:, None] * inverse[None, :]
    swap = np.zeros((2 * half, 2 * half), np.float32)
    for j in range(half):
        swap[half + j, j] = -1.0
        swap[j, half + j] = 1.0
    return (
        np.stack([np.cos(near), np.sin(near)]).astype(np.float32),
        np.stack([np.cos(far), np.sin(far)]).astype(np.float32),
        swap,
    )


def dot(a, b):
    return jnp.dot(a, b, preferred_element_type=F32)


def dot_nt(a, b, precision=None):
    return lax.dot_general(
        a, b, (((1,), (1,)), ((), ())), precision=precision, preferred_element_type=F32
    )


def kernel(
    sizes,
    rq_ref, rk_ref, rv_ref, ld_ref, gain_ref, mq_ref, kv_ref, rope_ref,
    near_r, far_r, swap_r, near_m, far_m, swap_m,
    ku_hbm, vu_hbm, ro_hbm, mo_hbm,
    out_ref, lw_ref,
    ku, vu, ro, mo,
    kvb, q_ref, m_ref, l_ref, acc_ref,
    dec_own, dec, st_own, st_in, pre_out, pre_in,
    gath, part, tin, osum, oin, intra_ref, rot_ref, grow_ref,
    w_sem, d_send, d_recv, s_send, s_recv, h_send, h_recv, k_send, k_recv,
    f_send, f_recv, y_send, g_send, g_recv, t_send, t_recv, o_send, o_recv,
):
    NP, NF, NT, RL, ML, G = sizes
    stride = NP // G
    NY = max(i for i in range(1, math.isqrt(NP) + 1) if NP % i == 0)
    NZ = NP // NY
    rows = rq_ref.shape[0]
    half = rows // NT
    r = st_own.shape[1]
    me = lax.axis_index("sp")
    fs = lax.axis_index("fs")
    tp = lax.axis_index("tp")
    z, y = lax.div(me, NY), lax.rem(me, NY)

    def remote(src, dst, ss, rs, axis, to):
        return pltpu.make_async_remote_copy(
            src_ref=src, dst_ref=dst, send_sem=ss, recv_sem=rs,
            device_id={axis: to}, device_id_type=MESH,
        )

    barrier = pltpu.get_barrier_semaphore()
    for axis, count, own in (("sp", NP, me), ("fs", NF, fs), ("tp", NT, tp)):
        for k in range(1, count):
            pl.semaphore_signal(
                barrier, inc=1, device_id={axis: lax.rem(own + k, count)}, device_id_type=MESH
            )

    wk, wv = ML * NOPE, ML * VDM
    weights = [
        pltpu.make_async_copy(
            ku_hbm.at[:, pl.ds(pl.multiple_of(tp * wk, 128), wk)], ku, w_sem.at[0]
        ),
        pltpu.make_async_copy(
            vu_hbm.at[:, pl.ds(pl.multiple_of(tp * wv, 128), wv)], vu, w_sem.at[1]
        ),
        pltpu.make_async_copy(ro_hbm, ro, w_sem.at[2]),
        pltpu.make_async_copy(mo_hbm, mo, w_sem.at[3]),
    ]
    for copy in weights:
        copy.start()

    def turn(near, far):
        cn, sn = near[0], near[1]
        co, so = far[0, pl.ds(me, 1), :], far[1, pl.ds(me, 1), :]
        return cn * co - sn * so, sn * co + cn * so

    cos_r, sin_r = turn(near_r, far_r)
    cos_m, sin_m = turn(near_m, far_m)

    def rot(x, cosine, sine, swap):
        return (x.astype(F32) * cosine + dot(x, swap[...]) * sine).astype(BF)

    own_rope = rot(rope_ref[...].astype(F32).T.astype(BF), cos_m, sin_m, swap_m)
    for t in range(NT):
        span = slice(t * half, (t + 1) * half)
        kvb[me, t, :, 0:KVR] = kv_ref[span, :]
        kvb[me, t, :, KVR:KW] = jnp.concatenate(
            [own_rope[span, :], jnp.zeros((half, KW - KVR - ROPE), BF)], axis=-1
        )

    ii = lax.broadcasted_iota(jnp.int32, (rows, rows), 0)
    jj = lax.broadcasted_iota(jnp.int32, (rows, rows), 1)
    low = ii >= jj
    ones_low = jnp.where(low, 1.0, 0.0).astype(F32)
    dec_own[...] = jnp.zeros_like(dec_own)
    dec_own[0:RL, :] = ld_ref[...]
    ld = dec_own[...]
    c_row = dot_nt(ld, ones_low, lax.Precision.HIGHEST)
    c_col = dot_nt(ones_low, ld, lax.Precision.HIGHEST)
    c_end = c_row[:, rows - 1 : rows]
    dec_own[...] = jnp.broadcast_to(jnp.exp(c_end), dec_own.shape)
    states, keys = [], []
    for h in range(RL):
        key = rot(rk_ref[:, h * QK : (h + 1) * QK], cos_r, sin_r, swap_r)
        keys.append(key)
        tail = jnp.exp(c_row[h : h + 1, rows - 1 : rows] - c_col[:, h : h + 1])
        scaled = (key.astype(F32) * tail).T.astype(BF)
        states.append(dot(scaled, rv_ref[:, h * VD : (h + 1) * VD]).astype(BF))
    for g in range(G):
        h, at = divmod(g * r, QK)
        st_own[g] = states[h][at : at + r, :]

    pl.semaphore_wait(barrier, (NP - 1) + (NF - 1) + (NT - 1))

    for g in range(G):
        to = g * stride

        @pl.when(jnp.logical_and(me != to, me < NP - 1))
        def _():
            remote(dec_own, dec.at[me], d_send.at[g], d_recv.at[me], "sp", to).start()
            remote(st_own.at[g], st_in.at[me], s_send.at[g], s_recv.at[me], "sp", to).start()

    def key_copy(to):
        return remote(
            kvb.at[me, tp], kvb.at[me, tp], k_send.at[to], k_recv.at[me], "sp", to
        )

    def key_targets(act):
        for k in range(1, NY):
            @pl.when(y + k < NY)
            def _():
                act(key_copy(me + k))

        @pl.loop(1, NZ)
        def _(d):
            @pl.when(z + d < NZ)
            def _():
                act(key_copy(me + d * NY))

    key_targets(lambda copy: copy.start())

    for h in range(RL):
        query = rot(rq_ref[:, h * QK : (h + 1) * QK], cos_r, sin_r, swap_r)
        rot_ref[h] = query
        gap = jnp.where(low, c_col[:, h : h + 1] - c_row[h : h + 1, :], 0.0)
        w = jnp.where(low, dot_nt(query, keys[h]) * (QK**-0.5) * jnp.exp(gap), 0.0).astype(BF)
        intra_ref[h] = dot(w, rv_ref[:, h * VD : (h + 1) * VD])
        grow_ref[h] = jnp.broadcast_to(
            jnp.exp(c_col[:, h : h + 1]) * (QK**-0.5), (rows, 128)
        )

    weights[0].wait()
    weights[1].wait()
    mq = mq_ref[...]
    width = NOPE + ROPE
    for h in range(ML):
        nope = mq[:, h * width : h * width + NOPE]
        span = slice(h * rows, (h + 1) * rows)
        q_ref[span, 0:KVR] = dot_nt(nope, ku[:, h * NOPE : (h + 1) * NOPE]).astype(BF)
        turned = rot(mq[:, h * width + NOPE : (h + 1) * width], cos_m, sin_m, swap_m)
        q_ref[span, KVR:KW] = jnp.concatenate(
            [turned, jnp.zeros((rows, KW - KVR - ROPE), BF)], axis=-1
        )

    def scores(at):
        block = kvb[at].reshape(rows, KW)
        return dot_nt(q_ref[...], block) * (width**-0.5), block[:, 0:KVR]

    s, latent = scores(me)
    hide = jnp.where(low, 0.0, -1e30).astype(F32)
    s = s + jnp.concatenate([hide] * ML, axis=0)
    top = jnp.max(s, axis=-1, keepdims=True)
    e = jnp.exp(s - top)
    m_ref[...] = jnp.broadcast_to(top, m_ref.shape)
    l_ref[...] = jnp.broadcast_to(jnp.sum(e, axis=-1, keepdims=True), l_ref.shape)
    acc_ref[...] = dot(e.astype(BF), latent)

    @pl.when(lax.rem(me, stride) == 0)
    def _():
        g = lax.div(me, stride)
        head = lax.div(g * r, QK)
        st_in[me] = st_own[g]
        dec[me] = dec_own[...]

        def scan(n, pre):
            pre_out[n] = pre.astype(BF)

            @pl.when(jnp.logical_and(n > 0, n != me))
            def _():
                remote(pre_out.at[n], pre_in.at[g], h_send.at[n], h_recv.at[g], "sp", n).start()

            @pl.when(jnp.logical_and(n < NP - 1, n != me))
            def _():
                remote(dec_own, dec.at[n], d_send.at[0], d_recv.at[n], "sp", n).wait_recv()
                remote(st_own.at[0], st_in.at[n], s_send.at[0], s_recv.at[n], "sp", n).wait_recv()

            factor = dec[n, pl.ds(head, 1), 0:1]
            return pre * factor + st_in[n].astype(F32)

        last = lax.fori_loop(0, NP - 1, scan, jnp.zeros((r, VD), F32))
        pre_out[NP - 1] = last.astype(BF)

        @pl.when(me != NP - 1)
        def _():
            remote(
                pre_out.at[NP - 1], pre_in.at[g], h_send.at[NP - 1], h_recv.at[g], "sp", NP - 1
            ).start()

        pre_in[g] = pre_out[me]

    def forward(at, k):
        to = lax.rem(tp + k, NT)
        return remote(
            kvb.at[at, tp], kvb.at[at, tp], f_send.at[k, at], f_recv.at[tp, at], "tp", to
        )

    def relay(at, k):
        to = z * NY + lax.rem(y + k, NY)
        return remote(
            kvb.at[at, tp], kvb.at[at, tp], y_send.at[k, at], k_recv.at[at], "sp", to
        )

    def landed(at):
        remote(kvb.at[at, tp], kvb.at[at, tp], k_send.at[at], k_recv.at[at], "sp", at).wait_recv()
        for k in range(1, NT):
            forward(at, k).start()

    def paired(at):
        for k in range(1, NT):
            src = lax.rem(tp + k, NT)
            remote(
                kvb.at[at, src], kvb.at[at, src], f_send.at[k, at], f_recv.at[src, at], "tp", src
            ).wait_recv()

    def attend(block):
        s = dot_nt(q_ref[...], block) * (width**-0.5)
        before = m_ref[:, 0:1]
        top = jnp.maximum(before, jnp.max(s, axis=-1, keepdims=True))
        e = jnp.exp(s - top)
        shrink = jnp.exp(before - top)
        total = l_ref[:, 0:1] * shrink + jnp.sum(e, axis=-1, keepdims=True)
        m_ref[...] = jnp.broadcast_to(top, m_ref.shape)
        l_ref[...] = jnp.broadcast_to(total, l_ref.shape)
        acc_ref[...] = acc_ref[...] * shrink + dot(e.astype(BF), block[:, 0:KVR])

    def direct(j):
        @pl.when(j <= z)
        def _():
            at = me - j * NY
            landed(at)
            for k in range(1, NY):
                relay(at, k).start()

    direct(1)
    for k in range(1, NY):
        @pl.when(y >= k)
        def _():
            landed(me - k)

    for k in range(1, NY):
        @pl.when(y >= k)
        def _():
            paired(me - k)
            attend(kvb[me - k].reshape(rows, KW))

    def line_landed(j):
        for k in range(1, NY):
            landed((z - j) * NY + lax.rem(y + k, NY))

    def line(j):
        direct(j + 1)

        @pl.when(j <= z)
        def _():
            first = (z - j) * NY

            @pl.when(j < NZ - 1)
            def _():
                line_landed(j)

            for k in range(NY):
                paired(first + lax.rem(y + k, NY))
            attend(kvb[pl.ds(first, NY)].reshape(NY * rows, KW))

    split = max(NZ - 1, 1)

    @pl.loop(1, split)
    def _(j):
        line(j)

    if NZ > 1:
        @pl.when(z == NZ - 1)
        def _():
            line_landed(NZ - 1)

    def heads_copy(kind, k):
        to = lax.rem(fs + k, NF)
        return remote(
            gath.at[fs, kind], gath.at[fs, kind], g_send.at[k, kind], g_recv.at[fs, kind], "fs", to
        )

    @pl.when(me > 0)
    def _():
        for g in range(G):
            @pl.when(me != g * stride)
            def _():
                remote(
                    pre_out.at[0], pre_in.at[g], h_send.at[0], h_recv.at[g], "sp", g * stride
                ).wait_recv()

    @pl.when(me == 0)
    def _():
        pre_in[...] = jnp.zeros_like(pre_in)

    per = G // RL
    for h in range(RL):
        state = pre_in[h * per : (h + 1) * per].reshape(QK, VD)
        kept = intra_ref[h] + dot(rot_ref[h], state) * grow_ref[h][:, 0:1]
        normed = kept * lax.rsqrt(jnp.mean(kept * kept, axis=-1, keepdims=True) + 1e-06)
        normed = normed * gain_ref[0:1, h * VD : (h + 1) * VD]
        gath[fs, 0, :, h * VD : (h + 1) * VD] = normed.astype(BF)
    for k in range(1, NF):
        heads_copy(0, k).start()

    @pl.loop(split, NZ)
    def _(j):
        line(j)

    for h in range(ML):
        span = slice(h * rows, (h + 1) * rows)
        total = l_ref[span, :]
        mean = (acc_ref[span, :] / total[:, 0:1]).astype(BF)
        gath[fs, 1, :, h * VDM : (h + 1) * VDM] = dot(mean, vu[:, h * VDM : (h + 1) * VDM]).astype(BF)
        lw_ref[h : h + 1, :] = (m_ref[span, :] + jnp.log(total)).T[0:1, :]
    for k in range(1, NF):
        heads_copy(1, k).start()

    weights[2].wait()
    weights[3].wait()

    cols = out_ref.shape[1] // NF
    piece = cols // CUTS

    def partial_copy(i, k):
        to = lax.rem(tp + k, NT)
        return remote(part.at[i, to], tin.at[tp, i], t_send.at[k, i], t_recv.at[tp, i], "tp", to)

    def project(s, ready):
        ready(0)
        base = dot(gath[s, 0], ro[...])
        ready(1)
        for c in range(CUTS):
            span = slice(c * piece, (c + 1) * piece)
            whole = (base[:, span] + dot(gath[s, 1], mo[:, span])).astype(BF)
            for t in range(NT):
                part[s * CUTS + c, t] = whole[t * half : (t + 1) * half, :]
            for k in range(1, NT):
                partial_copy(s * CUTS + c, k).start()

    def summed(i):
        total = part[i, tp].astype(F32)
        for k in range(1, NT):
            src = lax.rem(tp + k, NT)
            remote(part.at[i, 0], tin.at[src, i], t_send.at[k, i], t_recv.at[src, i], "tp", src).wait_recv()
            total = total + tin[src, i].astype(F32)
        return total.astype(BF)

    def place(s, c):
        return pl.ds(pl.multiple_of(s * cols + c * piece, 128), piece)

    project(fs, lambda kind: None)
    for c in range(CUTS):
        out_ref[:, place(fs, c)] = summed(fs * CUTS + c)
    for k in range(1, NF):
        s = lax.rem(fs + k, NF)

        def ready(kind):
            remote(
                gath.at[s, kind], gath.at[s, kind], g_send.at[k, kind], g_recv.at[s, kind], "fs", s
            ).wait_recv()

        project(s, ready)

    def back_copy(k, c):
        s = lax.rem(fs + k, NF)
        return remote(
            osum.at[s * CUTS + c], oin.at[fs * CUTS + c],
            o_send.at[k, c], o_recv.at[fs, c], "fs", s,
        )

    for k in range(1, NF):
        s = lax.rem(fs + k, NF)
        for c in range(CUTS):
            osum[s * CUTS + c] = summed(s * CUTS + c)
            back_copy(k, c).start()

    key_targets(lambda copy: copy.wait_send())

    @pl.loop(1, NZ)
    def _(j):
        @pl.when(j <= z)
        def _():
            for k in range(1, NY):
                relay(me - j * NY, k).wait_send()

    for g in range(G):
        @pl.when(jnp.logical_and(me != g * stride, me < NP - 1))
        def _():
            remote(dec_own, dec.at[me], d_send.at[g], d_recv.at[me], "sp", g * stride).wait_send()
            remote(st_own.at[g], st_in.at[me], s_send.at[g], s_recv.at[me], "sp", g * stride).wait_send()

    @pl.loop(1, NP)
    def _(d):
        @pl.when(d <= me)
        def _():
            for k in range(1, NT):
                forward(me - d, k).wait_send()

        @pl.when(jnp.logical_and(lax.rem(me, stride) == 0, d != me))
        def _():
            g = lax.div(me, stride)
            remote(pre_out.at[d], pre_in.at[g], h_send.at[d], h_recv.at[g], "sp", d).wait_send()

    for k in range(1, NF):
        for kind in range(2):
            heads_copy(kind, k).wait_send()
    for i in range(NF * CUTS):
        for k in range(1, NT):
            partial_copy(i, k).wait_send()
    for k in range(1, NF):
        for c in range(CUTS):
            back_copy(k, c).wait_send()
    for k in range(1, NF):
        s = lax.rem(fs + k, NF)
        for c in range(CUTS):
            i = s * CUTS + c
            remote(osum.at[i], oin.at[i], o_send.at[k, c], o_recv.at[s, c], "fs", s).wait_recv()
            out_ref[:, place(s, c)] = oin[i]


def on_device(
    counts,
    ret_query, ret_key, ret_value, log_decay, ret_gain, mla_query,
    kv_latent, rope_key, key_up, value_up, ret_out, mla_out,
):
    NP, NF, NT = counts
    rows = ret_query.shape[0]
    RL = ret_value.shape[2] // VD
    ML = mla_query.shape[2] // (NOPE + ROPE)
    G = min(NP, RL * QK // 16)
    r = RL * QK // G
    lines = max(i for i in range(1, math.isqrt(NP) + 1) if NP % i == 0)
    half = rows // NT
    cols = ret_out.shape[1]
    near_r, far_r, swap_r = tables(QK // 2, rows, NP)
    near_m, far_m, swap_m = tables(ROPE // 2, rows, NP)
    flat = lambda a: a.reshape(rows, a.shape[2])
    vm = pl.BlockSpec(memory_space=pltpu.VMEM)
    hbm = pl.BlockSpec(memory_space=pl.ANY)
    V = pltpu.VMEM
    D = pltpu.SemaphoreType.DMA
    out, lw = pl.pallas_call(
        functools.partial(kernel, (NP, NF, NT, RL, ML, G)),
        out_shape=(
            jax.ShapeDtypeStruct((half, cols * NF), BF),
            jax.ShapeDtypeStruct((ML, rows), F32),
        ),
        in_specs=[vm] * 14 + [hbm] * 4,
        out_specs=(vm, vm),
        scratch_shapes=[
            V((KVR, ML * NOPE), BF), V((KVR, ML * VDM), BF),
            V(ret_out.shape, BF), V(mla_out.shape, BF),
            V((NP, NT, half, KW), BF), V((ML * rows, KW), BF),
            V((ML * rows, 128), F32), V((ML * rows, 128), F32), V((ML * rows, KVR), F32),
            V((8, 128), F32), V((NP, 8, 128), F32),
            V((G, r, VD), BF), V((NP, r, VD), BF), V((NP, r, VD), BF), V((G, r, VD), BF),
            V((NF, 2, rows, ML * VDM), BF), V((NF * CUTS, NT, half, cols // CUTS), BF),
            V((NT, NF * CUTS, half, cols // CUTS), BF),
            V((NF * CUTS, half, cols // CUTS), BF), V((NF * CUTS, half, cols // CUTS), BF),
            V((RL, rows, VD), F32), V((RL, rows, QK), BF), V((RL, rows, 128), F32),
            D((4,)), D((G,)), D((NP,)), D((G,)), D((NP,)), D((NP,)), D((G,)), D((NP,)), D((NP,)),
            D((NT, NP)), D((NT, NP)), D((lines, NP)), D((NF, 2)), D((NF, 2)), D((NT, NF * CUTS)), D((NT, NF * CUTS)),
            D((NF, CUTS)), D((NF, CUTS)),
        ],
        compiler_params=pltpu.CompilerParams(collective_id=0, has_side_effects=True),
    )(
        flat(ret_query), flat(ret_key), flat(ret_value), log_decay.reshape(RL, rows),
        ret_gain.reshape(1, RL * VD), flat(mla_query), flat(kv_latent), flat(rope_key).T,
        jnp.asarray(near_r), jnp.asarray(far_r), jnp.asarray(swap_r, BF),
        jnp.asarray(near_m), jnp.asarray(far_m), jnp.asarray(swap_m, BF),
        key_up, value_up, ret_out, mla_out,
    )
    return out.reshape(half, 1, cols * NF), lw.reshape(1, ML, rows)


def solution(mesh):
    counts = tuple(mesh.shape[a] for a in ("sp", "fs", "tp"))
    wide = P("sp", "fs", "tp")
    in_specs = (
        wide, wide, wide, P("fs", "tp", "sp"), P("tp"), wide,
        P("sp", "fs", None), P("sp", "fs", None), P(), P(), P("tp", "fs"), P("tp", "fs"),
    )
    out_specs = (P(("sp", "tp"), "fs", None), P("fs", "tp", "sp"))
    return jax.shard_map(
        functools.partial(on_device, counts),
        mesh=mesh, in_specs=in_specs, out_specs=out_specs, check_vma=False,
    )
```

```python
import functools
import math

import jax
import jax.numpy as jnp
import numpy as np
from jax import lax
from jax.experimental import pallas as pl
from jax.experimental.pallas import tpu as pltpu
from jax.sharding import PartitionSpec as P

QK = 128
VD = 256
NOPE = 128
ROPE = 64
VDM = 128
KVR = 256
KW = 384
CUTS = 2
MESH = pl.DeviceIdType.MESH
BF = jnp.bfloat16
F32 = jnp.float32


def tables(half, rows, places):
    inverse = 1.0 / 10000.0 ** (np.arange(half) / half)
    inverse = np.concatenate([inverse, inverse])
    near = np.arange(rows)[:, None] * inverse[None, :]
    far = (np.arange(places) * rows)[:, None] * inverse[None, :]
    swap = np.zeros((2 * half, 2 * half), np.float32)
    for j in range(half):
        swap[half + j, j] = -1.0
        swap[j, half + j] = 1.0
    return (
        np.stack([np.cos(near), np.sin(near)]).astype(np.float32),
        np.stack([np.cos(far), np.sin(far)]).astype(np.float32),
        swap,
    )


def dot(a, b):
    return jnp.dot(a, b, preferred_element_type=F32)


def dot_nt(a, b, precision=None):
    return lax.dot_general(
        a, b, (((1,), (1,)), ((), ())), precision=precision, preferred_element_type=F32
    )


def kernel(
    sizes,
    rq_ref, rk_ref, rv_ref, ld_ref, gain_ref, mq_ref, kv_ref, rope_ref,
    near_r, far_r, swap_r, near_m, far_m, swap_m,
    ku_hbm, vu_hbm, ro_hbm, mo_hbm,
    out_ref, lw_ref,
    ku, vu, ro, mo,
    kvb, q_ref, m_ref, l_ref, acc_ref,
    dec_own, dec, st_own, st_in, pre_out, pre_in,
    gath, part, tin, osum, oin, intra_ref, rot_ref, grow_ref,
    w_sem, d_send, d_recv, s_send, s_recv, h_send, h_recv, k_send, k_recv,
    f_send, f_recv, y_send, g_send, g_recv, t_send, t_recv, o_send, o_recv,
):
    NP, NF, NT, RL, ML, G = sizes
    stride = NP // G
    NY = max(i for i in range(1, math.isqrt(NP) + 1) if NP % i == 0)
    NZ = NP // NY
    rows = rq_ref.shape[0]
    half = rows // NT
    r = st_own.shape[1]
    me = lax.axis_index("sp")
    fs = lax.axis_index("fs")
    tp = lax.axis_index("tp")
    z, y = lax.div(me, NY), lax.rem(me, NY)

    def remote(src, dst, ss, rs, axis, to):
        return pltpu.make_async_remote_copy(
            src_ref=src, dst_ref=dst, send_sem=ss, recv_sem=rs,
            device_id={axis: to}, device_id_type=MESH,
        )

    barrier = pltpu.get_barrier_semaphore()
    for axis, count, own in (("sp", NP, me), ("fs", NF, fs), ("tp", NT, tp)):
        for k in range(1, count):
            pl.semaphore_signal(
                barrier, inc=1, device_id={axis: lax.rem(own + k, count)}, device_id_type=MESH
            )

    wk, wv = ML * NOPE, ML * VDM
    weights = [
        pltpu.make_async_copy(
            ku_hbm.at[:, pl.ds(pl.multiple_of(tp * wk, 128), wk)], ku, w_sem.at[0]
        ),
        pltpu.make_async_copy(
            vu_hbm.at[:, pl.ds(pl.multiple_of(tp * wv, 128), wv)], vu, w_sem.at[1]
        ),
        pltpu.make_async_copy(ro_hbm, ro, w_sem.at[2]),
        pltpu.make_async_copy(mo_hbm, mo, w_sem.at[3]),
    ]
    for copy in weights:
        copy.start()

    def turn(near, far):
        cn, sn = near[0], near[1]
        co, so = far[0, pl.ds(me, 1), :], far[1, pl.ds(me, 1), :]
        return cn * co - sn * so, sn * co + cn * so

    cos_r, sin_r = turn(near_r, far_r)
    cos_m, sin_m = turn(near_m, far_m)

    def rot(x, cosine, sine, swap):
        return (x.astype(F32) * cosine + dot(x, swap[...]) * sine).astype(BF)

    own_rope = rot(rope_ref[...].astype(F32).T.astype(BF), cos_m, sin_m, swap_m)
    for t in range(NT):
        span = slice(t * half, (t + 1) * half)
        kvb[me, t, :, 0:KVR] = kv_ref[span, :]
        kvb[me, t, :, KVR:KW] = jnp.concatenate(
            [own_rope[span, :], jnp.zeros((half, KW - KVR - ROPE), BF)], axis=-1
        )

    ii = lax.broadcasted_iota(jnp.int32, (rows, rows), 0)
    jj = lax.broadcasted_iota(jnp.int32, (rows, rows), 1)
    low = ii >= jj
    ones_low = jnp.where(low, 1.0, 0.0).astype(F32)
    dec_own[...] = jnp.zeros_like(dec_own)
    dec_own[0:RL, :] = ld_ref[...]
    ld = dec_own[...]
    c_row = dot_nt(ld, ones_low, lax.Precision.HIGHEST)
    c_col = dot_nt(ones_low, ld, lax.Precision.HIGHEST)
    c_end = c_row[:, rows - 1 : rows]
    dec_own[...] = jnp.broadcast_to(jnp.exp(c_end), dec_own.shape)
    states, keys = [], []
    for h in range(RL):
        key = rot(rk_ref[:, h * QK : (h + 1) * QK], cos_r, sin_r, swap_r)
        keys.append(key)
        tail = jnp.exp(c_row[h : h + 1, rows - 1 : rows] - c_col[:, h : h + 1])
        scaled = (key.astype(F32) * tail).T.astype(BF)
        states.append(dot(scaled, rv_ref[:, h * VD : (h + 1) * VD]).astype(BF))
    for g in range(G):
        h, at = divmod(g * r, QK)
        st_own[g] = states[h][at : at + r, :]

    pl.semaphore_wait(barrier, (NP - 1) + (NF - 1) + (NT - 1))

    for g in range(G):
        to = g * stride

        @pl.when(jnp.logical_and(me != to, me < NP - 1))
        def _():
            remote(dec_own, dec.at[me], d_send.at[g], d_recv.at[me], "sp", to).start()
            remote(st_own.at[g], st_in.at[me], s_send.at[g], s_recv.at[me], "sp", to).start()

    def key_copy(to):
        return remote(
            kvb.at[me, tp], kvb.at[me, tp], k_send.at[to], k_recv.at[me], "sp", to
        )

    def key_targets(act):
        for k in range(1, NY):
            @pl.when(y + k < NY)
            def _():
                act(key_copy(me + k))

        @pl.loop(1, NZ)
        def _(d):
            @pl.when(z + d < NZ)
            def _():
                act(key_copy(me + d * NY))

    key_targets(lambda copy: copy.start())

    for h in range(RL):
        query = rot(rq_ref[:, h * QK : (h + 1) * QK], cos_r, sin_r, swap_r)
        rot_ref[h] = query
        gap = jnp.where(low, c_col[:, h : h + 1] - c_row[h : h + 1, :], 0.0)
        w = jnp.where(low, dot_nt(query, keys[h]) * (QK**-0.5) * jnp.exp(gap), 0.0).astype(BF)
        intra_ref[h] = dot(w, rv_ref[:, h * VD : (h + 1) * VD])
        grow_ref[h] = jnp.broadcast_to(
            jnp.exp(c_col[:, h : h + 1]) * (QK**-0.5), (rows, 128)
        )

    weights[0].wait()
    weights[1].wait()
    mq = mq_ref[...]
    width = NOPE + ROPE
    for h in range(ML):
        nope = mq[:, h * width : h * width + NOPE]
        span = slice(h * rows, (h + 1) * rows)
        q_ref[span, 0:KVR] = dot_nt(nope, ku[:, h * NOPE : (h + 1) * NOPE]).astype(BF)
        turned = rot(mq[:, h * width + NOPE : (h + 1) * width], cos_m, sin_m, swap_m)
        q_ref[span, KVR:KW] = jnp.concatenate(
            [turned, jnp.zeros((rows, KW - KVR - ROPE), BF)], axis=-1
        )

    def scores(at):
        block = kvb[at].reshape(rows, KW)
        return dot_nt(q_ref[...], block) * (width**-0.5), block[:, 0:KVR]

    s, latent = scores(me)
    hide = jnp.where(low, 0.0, -1e30).astype(F32)
    s = s + jnp.concatenate([hide] * ML, axis=0)
    top = jnp.max(s, axis=-1, keepdims=True)
    e = jnp.exp(s - top)
    m_ref[...] = jnp.broadcast_to(top, m_ref.shape)
    l_ref[...] = jnp.broadcast_to(jnp.sum(e, axis=-1, keepdims=True), l_ref.shape)
    acc_ref[...] = dot(e.astype(BF), latent)

    @pl.when(lax.rem(me, stride) == 0)
    def _():
        g = lax.div(me, stride)
        head = lax.div(g * r, QK)
        st_in[me] = st_own[g]
        dec[me] = dec_own[...]

        def scan(n, pre):
            pre_out[n] = pre.astype(BF)

            @pl.when(jnp.logical_and(n > 0, n != me))
            def _():
                remote(pre_out.at[n], pre_in.at[g], h_send.at[n], h_recv.at[g], "sp", n).start()

            @pl.when(jnp.logical_and(n < NP - 1, n != me))
            def _():
                remote(dec_own, dec.at[n], d_send.at[0], d_recv.at[n], "sp", n).wait_recv()
                remote(st_own.at[0], st_in.at[n], s_send.at[0], s_recv.at[n], "sp", n).wait_recv()

            factor = dec[n, pl.ds(head, 1), 0:1]
            return pre * factor + st_in[n].astype(F32)

        last = lax.fori_loop(0, NP - 1, scan, jnp.zeros((r, VD), F32))
        pre_out[NP - 1] = last.astype(BF)

        @pl.when(me != NP - 1)
        def _():
            remote(
                pre_out.at[NP - 1], pre_in.at[g], h_send.at[NP - 1], h_recv.at[g], "sp", NP - 1
            ).start()

        pre_in[g] = pre_out[me]

    def forward(at, k):
        to = lax.rem(tp + k, NT)
        return remote(
            kvb.at[at, tp], kvb.at[at, tp], f_send.at[k, at], f_recv.at[tp, at], "tp", to
        )

    def relay(at, k):
        to = z * NY + lax.rem(y + k, NY)
        return remote(
            kvb.at[at, tp], kvb.at[at, tp], y_send.at[k, at], k_recv.at[at], "sp", to
        )

    def landed(at):
        remote(kvb.at[at, tp], kvb.at[at, tp], k_send.at[at], k_recv.at[at], "sp", at).wait_recv()
        for k in range(1, NT):
            forward(at, k).start()

    def paired(at):
        for k in range(1, NT):
            src = lax.rem(tp + k, NT)
            remote(
                kvb.at[at, src], kvb.at[at, src], f_send.at[k, at], f_recv.at[src, at], "tp", src
            ).wait_recv()

    def attend(block):
        s = dot_nt(q_ref[...], block) * (width**-0.5)
        before = m_ref[:, 0:1]
        top = jnp.maximum(before, jnp.max(s, axis=-1, keepdims=True))
        e = jnp.exp(s - top)
        shrink = jnp.exp(before - top)
        total = l_ref[:, 0:1] * shrink + jnp.sum(e, axis=-1, keepdims=True)
        m_ref[...] = jnp.broadcast_to(top, m_ref.shape)
        l_ref[...] = jnp.broadcast_to(total, l_ref.shape)
        acc_ref[...] = acc_ref[...] * shrink + dot(e.astype(BF), block[:, 0:KVR])

    def direct(j):
        @pl.when(j <= z)
        def _():
            at = me - j * NY
            landed(at)
            for k in range(1, NY):
                relay(at, k).start()

    direct(1)
    for k in range(1, NY):
        @pl.when(y >= k)
        def _():
            landed(me - k)

    for k in range(1, NY):
        @pl.when(y >= k)
        def _():
            paired(me - k)
            attend(kvb[me - k].reshape(rows, KW))

    def line_landed(j):
        for k in range(1, NY):
            landed((z - j) * NY + lax.rem(y + k, NY))

    def line(j):
        direct(j + 1)

        @pl.when(j <= z)
        def _():
            first = (z - j) * NY

            line_landed(j)

            for k in range(NY):
                paired(first + lax.rem(y + k, NY))
            attend(kvb[pl.ds(first, NY)].reshape(NY * rows, KW))

    split = max(NZ // 2, 1)

    @pl.loop(1, split)
    def _(j):
        line(j)

    def heads_copy(kind, k):
        to = lax.rem(fs + k, NF)
        return remote(
            gath.at[fs, kind], gath.at[fs, kind], g_send.at[k, kind], g_recv.at[fs, kind], "fs", to
        )

    @pl.when(me > 0)
    def _():
        for g in range(G):
            @pl.when(me != g * stride)
            def _():
                remote(
                    pre_out.at[0], pre_in.at[g], h_send.at[0], h_recv.at[g], "sp", g * stride
                ).wait_recv()

    @pl.when(me == 0)
    def _():
        pre_in[...] = jnp.zeros_like(pre_in)

    per = G // RL
    for h in range(RL):
        state = pre_in[h * per : (h + 1) * per].reshape(QK, VD)
        kept = intra_ref[h] + dot(rot_ref[h], state) * grow_ref[h][:, 0:1]
        normed = kept * lax.rsqrt(jnp.mean(kept * kept, axis=-1, keepdims=True) + 1e-06)
        normed = normed * gain_ref[0:1, h * VD : (h + 1) * VD]
        gath[fs, 0, :, h * VD : (h + 1) * VD] = normed.astype(BF)
    for k in range(1, NF):
        heads_copy(0, k).start()

    @pl.loop(split, NZ)
    def _(j):
        line(j)

    for h in range(ML):
        span = slice(h * rows, (h + 1) * rows)
        total = l_ref[span, :]
        mean = (acc_ref[span, :] / total[:, 0:1]).astype(BF)
        gath[fs, 1, :, h * VDM : (h + 1) * VDM] = dot(mean, vu[:, h * VDM : (h + 1) * VDM]).astype(BF)
        lw_ref[h : h + 1, :] = (m_ref[span, :] + jnp.log(total)).T[0:1, :]
    for k in range(1, NF):
        heads_copy(1, k).start()

    weights[2].wait()
    weights[3].wait()

    cols = out_ref.shape[1] // NF
    piece = cols // CUTS

    def partial_copy(i, k):
        to = lax.rem(tp + k, NT)
        return remote(part.at[i, to], tin.at[tp, i], t_send.at[k, i], t_recv.at[tp, i], "tp", to)

    def project(s, ready):
        ready(0)
        base = dot(gath[s, 0], ro[...])
        ready(1)
        for c in range(CUTS):
            span = slice(c * piece, (c + 1) * piece)
            whole = (base[:, span] + dot(gath[s, 1], mo[:, span])).astype(BF)
            for t in range(NT):
                part[s * CUTS + c, t] = whole[t * half : (t + 1) * half, :]
            for k in range(1, NT):
                partial_copy(s * CUTS + c, k).start()

    def summed(i):
        total = part[i, tp].astype(F32)
        for k in range(1, NT):
            src = lax.rem(tp + k, NT)
            remote(part.at[i, 0], tin.at[src, i], t_send.at[k, i], t_recv.at[src, i], "tp", src).wait_recv()
            total = total + tin[src, i].astype(F32)
        return total.astype(BF)

    def place(s, c):
        return pl.ds(pl.multiple_of(s * cols + c * piece, 128), piece)

    project(fs, lambda kind: None)
    for c in range(CUTS):
        out_ref[:, place(fs, c)] = summed(fs * CUTS + c)
    for k in range(1, NF):
        s = lax.rem(fs + k, NF)

        def ready(kind):
            remote(
                gath.at[s, kind], gath.at[s, kind], g_send.at[k, kind], g_recv.at[s, kind], "fs", s
            ).wait_recv()

        project(s, ready)

    def back_copy(k, c):
        s = lax.rem(fs + k, NF)
        return remote(
            osum.at[s * CUTS + c], oin.at[fs * CUTS + c],
            o_send.at[k, c], o_recv.at[fs, c], "fs", s,
        )

    for k in range(1, NF):
        s = lax.rem(fs + k, NF)
        for c in range(CUTS):
            osum[s * CUTS + c] = summed(s * CUTS + c)
            back_copy(k, c).start()

    key_targets(lambda copy: copy.wait_send())

    @pl.loop(1, NZ)
    def _(j):
        @pl.when(j <= z)
        def _():
            for k in range(1, NY):
                relay(me - j * NY, k).wait_send()

    for g in range(G):
        @pl.when(jnp.logical_and(me != g * stride, me < NP - 1))
        def _():
            remote(dec_own, dec.at[me], d_send.at[g], d_recv.at[me], "sp", g * stride).wait_send()
            remote(st_own.at[g], st_in.at[me], s_send.at[g], s_recv.at[me], "sp", g * stride).wait_send()

    @pl.loop(1, NP)
    def _(d):
        @pl.when(d <= me)
        def _():
            for k in range(1, NT):
                forward(me - d, k).wait_send()

        @pl.when(jnp.logical_and(lax.rem(me, stride) == 0, d != me))
        def _():
            g = lax.div(me, stride)
            remote(pre_out.at[d], pre_in.at[g], h_send.at[d], h_recv.at[g], "sp", d).wait_send()

    for k in range(1, NF):
        for kind in range(2):
            heads_copy(kind, k).wait_send()
    for i in range(NF * CUTS):
        for k in range(1, NT):
            partial_copy(i, k).wait_send()
    for k in range(1, NF):
        for c in range(CUTS):
            back_copy(k, c).wait_send()
    for k in range(1, NF):
        s = lax.rem(fs + k, NF)
        for c in range(CUTS):
            i = s * CUTS + c
            remote(osum.at[i], oin.at[i], o_send.at[k, c], o_recv.at[s, c], "fs", s).wait_recv()
            out_ref[:, place(s, c)] = oin[i]


def on_device(
    counts,
    ret_query, ret_key, ret_value, log_decay, ret_gain, mla_query,
    kv_latent, rope_key, key_up, value_up, ret_out, mla_out,
):
    NP, NF, NT = counts
    rows = ret_query.shape[0]
    RL = ret_value.shape[2] // VD
    ML = mla_query.shape[2] // (NOPE + ROPE)
    G = min(NP, RL * QK // 16)
    r = RL * QK // G
    lines = max(i for i in range(1, math.isqrt(NP) + 1) if NP % i == 0)
    half = rows // NT
    cols = ret_out.shape[1]
    near_r, far_r, swap_r = tables(QK // 2, rows, NP)
    near_m, far_m, swap_m = tables(ROPE // 2, rows, NP)
    flat = lambda a: a.reshape(rows, a.shape[2])
    vm = pl.BlockSpec(memory_space=pltpu.VMEM)
    hbm = pl.BlockSpec(memory_space=pl.ANY)
    V = pltpu.VMEM
    D = pltpu.SemaphoreType.DMA
    out, lw = pl.pallas_call(
        functools.partial(kernel, (NP, NF, NT, RL, ML, G)),
        out_shape=(
            jax.ShapeDtypeStruct((half, cols * NF), BF),
            jax.ShapeDtypeStruct((ML, rows), F32),
        ),
        in_specs=[vm] * 14 + [hbm] * 4,
        out_specs=(vm, vm),
        scratch_shapes=[
            V((KVR, ML * NOPE), BF), V((KVR, ML * VDM), BF),
            V(ret_out.shape, BF), V(mla_out.shape, BF),
            V((NP, NT, half, KW), BF), V((ML * rows, KW), BF),
            V((ML * rows, 128), F32), V((ML * rows, 128), F32), V((ML * rows, KVR), F32),
            V((8, 128), F32), V((NP, 8, 128), F32),
            V((G, r, VD), BF), V((NP, r, VD), BF), V((NP, r, VD), BF), V((G, r, VD), BF),
            V((NF, 2, rows, ML * VDM), BF), V((NF * CUTS, NT, half, cols // CUTS), BF),
            V((NT, NF * CUTS, half, cols // CUTS), BF),
            V((NF * CUTS, half, cols // CUTS), BF), V((NF * CUTS, half, cols // CUTS), BF),
            V((RL, rows, VD), F32), V((RL, rows, QK), BF), V((RL, rows, 128), F32),
            D((4,)), D((G,)), D((NP,)), D((G,)), D((NP,)), D((NP,)), D((G,)), D((NP,)), D((NP,)),
            D((NT, NP)), D((NT, NP)), D((lines, NP)), D((NF, 2)), D((NF, 2)), D((NT, NF * CUTS)), D((NT, NF * CUTS)),
            D((NF, CUTS)), D((NF, CUTS)),
        ],
        compiler_params=pltpu.CompilerParams(collective_id=0, has_side_effects=True),
    )(
        flat(ret_query), flat(ret_key), flat(ret_value), log_decay.reshape(RL, rows),
        ret_gain.reshape(1, RL * VD), flat(mla_query), flat(kv_latent), flat(rope_key).T,
        jnp.asarray(near_r), jnp.asarray(far_r), jnp.asarray(swap_r, BF),
        jnp.asarray(near_m), jnp.asarray(far_m), jnp.asarray(swap_m, BF),
        key_up, value_up, ret_out, mla_out,
    )
    return out.reshape(half, 1, cols * NF), lw.reshape(1, ML, rows)


def solution(mesh):
    counts = tuple(mesh.shape[a] for a in ("sp", "fs", "tp"))
    wide = P("sp", "fs", "tp")
    in_specs = (
        wide, wide, wide, P("fs", "tp", "sp"), P("tp"), wide,
        P("sp", "fs", None), P("sp", "fs", None), P(), P(), P("tp", "fs"), P("tp", "fs"),
    )
    out_specs = (P(("sp", "tp"), "fs", None), P("fs", "tp", "sp"))
    return jax.shard_map(
        functools.partial(on_device, counts),
        mesh=mesh, in_specs=in_specs, out_specs=out_specs, check_vma=False,
    )
```
